32 devices in a mesh: sp: 8 (over z, x), tp: 4 (over y, core).
Axes of the slice: x: 2, y: 2, z: 4, core: 2. Of those that a mesh axis runs over, the one named last changes fastest.
Arguments:
- tokens: bfloat16 [4096, 2048], P('sp', 'tp'), may hold values from -400 to 400
- lru_in: bfloat16 [2048, 1024], P(None, 'tp'), may hold values from -0.125 to 0.125
- lru_gate_in: bfloat16 [2048, 1024], P(None, 'tp'), may hold values from -0.125 to 0.125
- query_w: bfloat16 [2048, 1024], P(None, 'tp'), may hold values from -1 to 1
- key_w: bfloat16 [2048, 1024], P(None, 'tp'), may hold values from -10 to 10
- value_w: bfloat16 [2048, 1024], P(None, 'tp'), may hold values from -0.125 to 0.125
- conv_weight: bfloat16 [4, 1024], replicated, may hold values from -3 to 3
- recur_gate_w: bfloat16 [16, 64, 64], replicated, may hold values from -0.75 to 0.75
- input_gate_w: bfloat16 [16, 64, 64], replicated, may hold values from -0.75 to 0.75
- rate_param: float32 [1024], replicated, may hold values from 0 to 16
- decay_extra: float32 [4096, 1024], P('sp', 'tp'), may hold values from -2 to 0
- forget_cum: float32 [4096, 8], P('sp', 'tp'), may hold values from -386 to 0, as said below
- out_lru: bfloat16 [1024, 2048], P('tp'), may hold values from -0.1875 to 0.1875
- out_fox: bfloat16 [1024, 2048], P('tp'), may hold values from -0.1875 to 0.1875
Outputs:
- mixed_out: bfloat16 [4096, 2048], P('sp', 'tp')
The draws below stay inside these ranges and needn't reach their ends.
Inputs may be any that keep to these rules, and one draw needn't show every extreme that they name: `forget_cum`: non-increasing along positions in every head.
All inputs are finite; a program needn't handle non-finite values.
Results may differ from the reference program's by a relative error of at most 0.014.
Values may be sent and summed in bfloat16 or wider, within the bound.
A program may use at most 64 MiB of HBM per device.

```python
import math
import jax
import jax.numpy as jnp
from jax import lax

D = 2048
LRU_W = 1024
LRU_BLOCKS = 16
BLOCK_W = 64
CONV_W = 4
FOX_HEADS = 8
HEAD_DIM = 128
FOX_W = 1024
TOKENS_PER_SHARD = 512
SEQUENCE_TOKENS = 4096


decay_sharpness = 8.0


def draw_tokens(key, part):
    random_subkeys = jax.random.split(key, 4)
    feature_scale = jnp.exp(jnp.linspace(0.0, math.log(4.0), D) + jax.random.uniform(random_subkeys[0], (D,), jnp.float32, -0.5, 0.5))
    row_scale = jnp.exp(jax.random.uniform(random_subkeys[1], (SEQUENCE_TOKENS, 1), jnp.float32, 0.0, math.log(10.0)))
    reference_level = jax.random.truncated_normal(random_subkeys[2], -4.0, 4.0, (SEQUENCE_TOKENS, D), jnp.float32)
    return (reference_level * feature_scale[None, :] * row_scale).astype(jnp.bfloat16)


def shared_query(key):
    return jax.random.truncated_normal(jax.random.fold_in(key, 11), -6.0, 6.0, (D, FOX_W), jnp.float32) * D ** (-0.5)


def draw_query_w(key, part):
    return shared_query(key).astype(jnp.bfloat16)


def draw_key_w(key, part):
    independent = jax.random.truncated_normal(jax.random.fold_in(key, 12), -6.0, 6.0, (D, FOX_W), jnp.float32) * D ** (-0.5)
    combined = 3.0 * independent
    return combined.astype(jnp.bfloat16)


def draw_rate_param(key, part):
    random_subkeys = jax.random.split(key, 3)
    ranking = jax.random.permutation(random_subkeys[0], LRU_W)
    slow_mask = ranking < LRU_W // 2
    slow_rate = jnp.exp(jax.random.uniform(random_subkeys[1], (LRU_W,), jnp.float32, math.log(0.2), math.log(0.8))) / (0.5 * decay_sharpness * SEQUENCE_TOKENS)
    fast_len = jnp.exp(jax.random.uniform(random_subkeys[2], (LRU_W,), jnp.float32, math.log(TOKENS_PER_SHARD / 16.0), math.log(TOKENS_PER_SHARD / 5.0)))
    fast_rate = 1.0 / (0.5 * decay_sharpness * fast_len)
    softplus_value = jnp.where(slow_mask, slow_rate, fast_rate)
    return -jnp.log(jnp.expm1(softplus_value))


def draw_decay_extra(key, part):
    random_subkeys = jax.random.split(key, 4)
    multiplier = jnp.exp(jax.random.uniform(random_subkeys[0], (SEQUENCE_TOKENS // TOKENS_PER_SHARD,), jnp.float32, math.log(0.4), math.log(1.6)))
    jaggedness = jax.random.uniform(random_subkeys[1], (SEQUENCE_TOKENS, LRU_W), jnp.float32, 0.2, 1.8)
    reference_level = -jnp.repeat(multiplier, TOKENS_PER_SHARD)[:, None] * jaggedness * (0.4 / SEQUENCE_TOKENS)
    spike_position = jax.random.randint(random_subkeys[2], (3,), 0, SEQUENCE_TOKENS)
    spike_penalty = jnp.log(jax.random.uniform(random_subkeys[3], (3,), jnp.float32, 0.6, 0.8))
    spike_events = jnp.zeros((SEQUENCE_TOKENS,), jnp.float32).at[spike_position].add(spike_penalty)
    return reference_level + spike_events[:, None]


def draw_forget_cum(key, part):
    random_subkeys = jax.random.split(key, 7)
    ranking = jax.random.permutation(random_subkeys[0], FOX_HEADS)
    slow_mask = ranking < FOX_HEADS // 2
    slow_rate = jnp.exp(jax.random.uniform(random_subkeys[1], (FOX_HEADS,), jnp.float32, math.log(0.3), math.log(1.0))) / SEQUENCE_TOKENS
    fast_len = jnp.exp(jax.random.uniform(random_subkeys[2], (FOX_HEADS,), jnp.float32, math.log(TOKENS_PER_SHARD / 16.0), math.log(TOKENS_PER_SHARD / 5.0)))
    head_decay_rate = jnp.where(slow_mask, slow_rate, 1.0 / fast_len)
    multiplier = jnp.exp(jax.random.uniform(random_subkeys[3], (SEQUENCE_TOKENS // TOKENS_PER_SHARD,), jnp.float32, math.log(0.4), math.log(1.6)))
    jaggedness = jax.random.uniform(random_subkeys[4], (SEQUENCE_TOKENS, FOX_HEADS), jnp.float32, 0.2, 1.8)
    spike_position = jax.random.randint(random_subkeys[5], (3,), 0, SEQUENCE_TOKENS)
    spike_penalty = jnp.log(jax.random.uniform(random_subkeys[6], (3,), jnp.float32, 0.6, 0.8))
    spike_events = jnp.zeros((SEQUENCE_TOKENS,), jnp.float32).at[spike_position].add(spike_penalty)
    logarithmic_steps = -head_decay_rate[None, :] * jnp.repeat(multiplier, TOKENS_PER_SHARD)[:, None] * jaggedness + spike_events[:, None]
    return jnp.cumsum(logarithmic_steps, axis=0)


def strengthened(values, own_key, source, target, parts, factor):
    def block_of(dim):
        return (jnp.arange(values.shape[dim]) // (values.shape[dim] // parts)).reshape((-1,) + (1,) * (values.ndim - 1 - dim))

    one_side = jax.random.permutation(own_key, parts)[block_of(target)]
    far = (block_of(target) + parts // 2) % parts
    return jnp.where((block_of(source) == one_side) | (block_of(source) == far), factor * values, values)


def block_levels(key, extent, cuts, smallest, top_value):
    level = 1.0
    for dim, parts in cuts:
        heights = jax.random.uniform(jax.random.fold_in(jax.random.fold_in(key, 6), dim), (parts,), jnp.float32, smallest / len(cuts), top_value / len(cuts))
        level = level * jnp.repeat(jnp.exp(heights), extent[dim] // parts).reshape((-1,) + (1,) * (len(extent) - 1 - dim))
    return level


def centred(own_key, extent, deviation, most, cuts=(), dtype=jnp.bfloat16):
    array = jax.random.normal(own_key, extent, jnp.float32) * deviation
    if len(cuts) > 0:
        array = block_levels(own_key, extent, cuts, -0.22, 0.18) * array
    return jnp.clip(array, min=-most, max=most).astype(dtype)


def noise_with(rng, extent, deviation, reach, shards, heavy, kind=jnp.bfloat16):
    values = deviation * jax.random.normal(rng, extent, jnp.float32)
    if shards:
        values = values * block_levels(rng, extent, shards, -0.22, 0.18)
    return jnp.clip(strengthened(values, jax.random.fold_in(rng, 3), *heavy), -reach, reach).astype(kind)


def setup_inputs(seed: int = 0) -> dict:
    streams_of = jax.random.split(jax.random.key(seed), 15)
    tokens = draw_tokens(jax.random.fold_in(streams_of[14], 71), 0)
    lru_in = centred(streams_of[1], (D, LRU_W), D ** -0.5, 0.125, ((1, 4),))
    lru_gate_in = centred(streams_of[2], (D, LRU_W), D ** -0.5, 0.125, ((1, 4),))
    query_w = draw_query_w(jax.random.fold_in(streams_of[14], 71), 0)
    key_w = draw_key_w(jax.random.fold_in(streams_of[14], 71), 0)
    value_w = centred(streams_of[5], (D, FOX_W), D ** -0.5, 0.125, ((1, 4),))
    conv_weight = centred(streams_of[6], (CONV_W, LRU_W), CONV_W ** -0.5, 3.0)
    recur_gate_w = centred(streams_of[7], (LRU_BLOCKS, BLOCK_W, BLOCK_W), BLOCK_W ** -0.5, 0.75)
    input_gate_w = centred(streams_of[8], (LRU_BLOCKS, BLOCK_W, BLOCK_W), BLOCK_W ** -0.5, 0.75)
    rate_param = draw_rate_param(jax.random.fold_in(streams_of[14], 71), 0)
    decay_extra = draw_decay_extra(jax.random.fold_in(streams_of[14], 71), 0)
    forget_cum = draw_forget_cum(jax.random.fold_in(streams_of[14], 71), 0)
    out_lru = noise_with(streams_of[12], (LRU_W, D), (LRU_W + FOX_W) ** -0.5, 0.1875, ((0, 4),), (0, 1, 4, 2.0))
    out_fox = noise_with(streams_of[13], (FOX_W, D), (LRU_W + FOX_W) ** -0.5, 0.1875, ((0, 4),), (0, 1, 4, 2.0))
    return {"tokens": tokens, "lru_in": lru_in, "lru_gate_in": lru_gate_in, "query_w": query_w, "key_w": key_w, "value_w": value_w, "conv_weight": conv_weight, "recur_gate_w": recur_gate_w, "input_gate_w": input_gate_w, "rate_param": rate_param, "decay_extra": decay_extra, "forget_cum": forget_cum, "out_lru": out_lru, "out_fox": out_fox}


decay_sharpness = 8.0
epsilon_norm = 1e-06

def combine_pairs(earlier, later):
    decay_one, state_one = earlier
    decay_two, state_two = later
    return (decay_one * decay_two, decay_two * state_one + state_two)

def reference(tokens, lru_in, lru_gate_in, query_w, key_w, value_w, conv_weight, recur_gate_w, input_gate_w, rate_param, decay_extra, forget_cum, out_lru, out_fox):
    token_f32 = tokens.astype(jnp.float32)
    row_scale = lax.rsqrt(lax.optimization_barrier(jnp.mean(token_f32 * token_f32, axis=1, keepdims=True)) + epsilon_norm)

    def project(weight):
        return (jnp.dot(tokens, weight, preferred_element_type=jnp.float32) * row_scale).astype(jnp.bfloat16)
    lru_input = project(lru_in)
    gate_input = project(lru_gate_in)
    queries = project(query_w)
    keys_all = project(key_w)
    values_all = project(value_w)
    padded = jnp.pad(lru_input, ((CONV_W - 1, 0), (0, 0)))
    conv_sum = jnp.zeros((SEQUENCE_TOKENS, LRU_W), jnp.float32)
    for tap_idx in range(CONV_W):
        conv_sum = conv_sum + conv_weight[tap_idx].astype(jnp.float32)[None, :] * padded[tap_idx:tap_idx + SEQUENCE_TOKENS].astype(jnp.float32)
    conv_out = conv_sum.astype(jnp.bfloat16)
    blocked = conv_out.astype(jnp.float32).reshape(SEQUENCE_TOKENS, LRU_BLOCKS, BLOCK_W)
    recur_gate = jax.nn.sigmoid(jnp.einsum('tnc,ncd->tnd', blocked, recur_gate_w.astype(jnp.float32)).reshape(SEQUENCE_TOKENS, LRU_W))
    input_gate = jax.nn.sigmoid(jnp.einsum('tnc,ncd->tnd', blocked, input_gate_w.astype(jnp.float32)).reshape(SEQUENCE_TOKENS, LRU_W))
    log_decay = -decay_sharpness * jax.nn.softplus(-rate_param)[None, :] * recur_gate + decay_extra
    driven = jnp.sqrt(-jnp.expm1(2.0 * log_decay)) * input_gate * conv_out.astype(jnp.float32)
    unused_decay, states = lax.associative_scan(combine_pairs, (jnp.exp(log_decay), driven), axis=0)
    lru_out = (states * jax.nn.gelu(gate_input.astype(jnp.float32))).astype(jnp.bfloat16)
    block_len = math.gcd(SEQUENCE_TOKENS, 512)
    block_count = SEQUENCE_TOKENS // block_len
    positions = jnp.arange(SEQUENCE_TOKENS).astype(jnp.int32)
    score_scale = HEAD_DIM ** (-0.5)
    heads_q = queries.reshape(SEQUENCE_TOKENS, FOX_HEADS, HEAD_DIM).transpose(1, 0, 2)
    heads_k = keys_all.reshape(SEQUENCE_TOKENS, FOX_HEADS, HEAD_DIM).transpose(1, 0, 2)
    heads_v = values_all.reshape(SEQUENCE_TOKENS, FOX_HEADS, HEAD_DIM).transpose(1, 0, 2)
    heads_c = forget_cum.T

    def one_head(entries):
        head_q, head_k, head_v, head_c = entries
        query_blocks = head_q.reshape(block_count, block_len, HEAD_DIM)
        cum_blocks = head_c.reshape(block_count, block_len)
        pos_blocks = positions.reshape(block_count, block_len)

        def one_block(block_entries):
            block_q, block_c, block_pos = block_entries
            scores = jnp.dot(block_q, head_k.T, preferred_element_type=jnp.float32) * score_scale
            scores = scores + block_c[:, None] - head_c[None, :]
            causal = block_pos[:, None] >= positions[None, :]
            scores = jnp.where(causal, scores, -jnp.inf)
            maxima = lax.optimization_barrier(jnp.max(scores, axis=1, keepdims=True))
            probs = jnp.where(causal, jnp.exp(scores - maxima), 0.0)
            totals = lax.optimization_barrier(jnp.sum(probs, axis=1, keepdims=True))
            weighted = jnp.dot(probs.astype(jnp.bfloat16), head_v, preferred_element_type=jnp.float32)
            return (weighted / totals).astype(jnp.bfloat16)
        return lax.map(one_block, (query_blocks, cum_blocks, pos_blocks)).reshape(SEQUENCE_TOKENS, HEAD_DIM)
    fox_heads = lax.map(one_head, (heads_q, heads_k, heads_v, heads_c))
    fox_out = fox_heads.transpose(1, 0, 2).reshape(SEQUENCE_TOKENS, FOX_W)
    mixed_out = jnp.dot(lru_out, out_lru, preferred_element_type=jnp.float32) + jnp.dot(fox_out, out_fox, preferred_element_type=jnp.float32)
    return mixed_out.astype(jnp.bfloat16)
```

```python
import functools

import jax
import jax.numpy as jnp
from jax import lax
from jax.experimental import pallas as pl
from jax.experimental.pallas import tpu as pltpu
from jax.sharding import PartitionSpec as P

HEAD_DIM = 128
decay_sharpness = 8.0
epsilon_norm = 1e-06
MESH = pl.DeviceIdType.MESH
F32 = jnp.float32
BF16 = jnp.bfloat16


def one_minus_exp(w):
    u = -w
    series = 1.0 - u / 9.0
    for n in range(8, 1, -1):
        series = 1.0 - u / n * series
    return jnp.where(u < 0.5, u * series, 1.0 - jnp.exp(w))


def remote(src, dst, send_sem, recv_sem, device):
    return pltpu.make_async_remote_copy(
        src_ref=src,
        dst_ref=dst,
        send_sem=send_sem,
        recv_sem=recv_sem,
        device_id=device,
        device_id_type=MESH,
    )


def kernel(
    SP,
    TP,
    X,
    tokens,
    lru_in,
    gate_in,
    query_w,
    key_w,
    value_w,
    conv_w,
    rg_w,
    ig_w,
    rate,
    decay_extra,
    forget,
    out_lru,
    out_fox,
    out,
    tok_buf,
    w_buf,
    acc,
    sq,
    lru_ref,
    halo,
    pad,
    bd_r,
    bd_i,
    gate_ref,
    q_ref,
    decay_buf,
    prefix_ref,
    local_ref,
    ends,
    incoming,
    kv_buf,
    cum_buf,
    cum_pad,
    m_ref,
    l_ref,
    o_ref,
    wl_buf,
    wf_buf,
    br_lru,
    br_fox,
    oacc,
    load_sem,
    tsend,
    tfwd,
    trecv,
    hsend,
    hrecv,
    esend,
    erecv,
    zsend,
    xsend,
    kvrecv,
    wsend,
    wrecv,
    lsend,
    lrecv,
    fsend,
    ffwd,
    frecv,
):
    rows, dcols = tokens.shape
    D, lw = lru_in.shape
    fw = query_w.shape[1]
    H = fw // HEAD_DIM
    oc = out.shape[1]
    Y = TP // 2
    Z = SP // X
    CH = tsend.shape[1]
    rc = rows // CH
    sp = lax.axis_index("sp")
    tp = lax.axis_index("tp")
    z = lax.div(sp, X)
    x = lax.rem(sp, X)
    partner = tp + 1 - 2 * lax.rem(tp, 2)
    far = [lax.rem(tp + 2 * k, TP) for k in range(Y)]
    pfar = [lax.rem(partner + 2 * k, TP) for k in range(Y)]
    offs = [0, lw, lw + fw, lw + 2 * fw, 2 * lw + 2 * fw, 2 * lw + 3 * fw]

    barrier = pltpu.get_barrier_semaphore()
    for k in range(1, SP):
        pl.semaphore_signal(
            barrier, inc=1, device_id={"sp": lax.rem(sp + k, SP)}, device_id_type=MESH
        )
    for k in range(1, TP):
        pl.semaphore_signal(
            barrier, inc=1, device_id={"tp": lax.rem(tp + k, TP)}, device_id_type=MESH
        )
    loads = []
    for i, w in enumerate((lru_in, key_w, value_w, gate_in, query_w)):
        c = pltpu.make_async_copy(w, w_buf.at[:, offs[i] : offs[i + 1]], load_sem.at[i])
        c.start()
        loads.append(c)
    mine = pl.ds(pl.multiple_of(tp * oc, 128), oc)
    own_loads = [
        pltpu.make_async_copy(decay_extra, decay_buf, load_sem.at[5]),
        pltpu.make_async_copy(out_lru.at[:, mine], wl_buf.at[tp], load_sem.at[6]),
        pltpu.make_async_copy(out_fox.at[:, mine], wf_buf.at[tp], load_sem.at[7]),
    ]
    for c in own_loads:
        c.start()
    pl.semaphore_wait(barrier, SP - 1 + TP - 1)

    pending = []

    def chunk(c):
        return pl.ds(c * rc, rc)

    for c in range(CH):
        for k in range(1, Y):
            s = remote(
                tokens.at[chunk(c)],
                tok_buf.at[tp, chunk(c)],
                tsend.at[k, c],
                trecv.at[tp, c],
                {"tp": far[k]},
            )
            s.start()
            pending.append(s)
    for c in range(CH):
        s = remote(
            tokens.at[chunk(c)],
            tok_buf.at[tp, chunk(c)],
            tsend.at[0, c],
            trecv.at[tp, c],
            {"tp": partner},
        )
        s.start()
        pending.append(s)

    bw = rg_w.shape[1]
    nb = lw // bw
    bd_r[...] = jnp.zeros_like(bd_r)
    bd_i[...] = jnp.zeros_like(bd_i)
    for n in range(nb):
        sl = pl.ds(n * bw, bw)
        bd_r[sl, sl] = rg_w[tp * nb + n]
        bd_i[sl, sl] = ig_w[tp * nb + n]
    cum_pad[...] = jnp.zeros_like(cum_pad)
    cum_pad[:, 0:H] = forget[...]
    cum_buf[sp] = cum_pad[...].T[0:8, :]

    for c in loads:
        c.wait()

    def project(val, src, r, first=False):
        w_rows = pl.ds(pl.multiple_of(src * dcols, dcols), dcols)
        v32 = val.astype(F32)
        part = jnp.sum(v32 * v32, axis=1, keepdims=True)
        dot = jnp.dot(val, w_buf[w_rows, :], preferred_element_type=F32)
        if first:
            sq[r, :] = part
            acc[r, :] = dot
        else:
            sq[r, :] += part
            acc[r, :] += dot

    def tok_wait(src, c):
        ref = tok_buf.at[src, chunk(c)]
        remote(ref, ref, tsend.at[0, c], trecv.at[src, c], {"tp": partner}).wait_recv()

    for c in range(CH):
        project(tokens[chunk(c), :], tp, chunk(c), True)
    for c in range(CH):
        tok_wait(partner, c)
        project(tok_buf[partner, chunk(c), :], partner, chunk(c))
    for c in range(CH):
        for k in range(1, Y):
            tok_wait(far[k], c)
            ref = tok_buf.at[far[k], chunk(c)]
            s = remote(ref, ref, tfwd.at[k, c], trecv.at[far[k], c], {"tp": partner})
            s.start()
            pending.append(s)
            project(tok_buf[far[k], chunk(c), :], far[k], chunk(c))
        for k in range(1, Y):
            tok_wait(pfar[k], c)
            project(tok_buf[pfar[k], chunk(c), :], pfar[k], chunk(c))

    row_scale = lax.rsqrt(sq[...] / D + epsilon_norm)

    def scaled(i, n=1):
        return (acc[:, offs[i] : offs[i + n]] * row_scale).astype(BF16)

    lru_ref[...] = scaled(0)
    hb = halo.shape[0]
    halo_copy = remote(
        lru_ref.at[pl.ds(rows - hb, hb)],
        halo,
        hsend.at[0],
        hrecv.at[0],
        {"sp": lax.rem(sp + 1, SP)},
    )

    @pl.when(sp < SP - 1)
    def _():
        halo_copy.start()

    kv_buf[sp] = scaled(1, 2)

    def block_copies(j, a, send_sem, device):
        return (
            remote(kv_buf.at[j], kv_buf.at[j], send_sem.at[a, 0], kvrecv.at[j, 0], device),
            remote(cum_buf.at[j], cum_buf.at[j], send_sem.at[a, 1], kvrecv.at[j, 1], device),
        )

    def z_copies(dz):
        j = (z - dz) * X + x
        return block_copies(j, dz, zsend, {"sp": lax.rem(sp + X, SP)})

    def x_copies(dz, dx):
        j = (z - dz) * X + x
        xo = lax.rem(x + dx, X)
        return block_copies(j, dz, xsend.at[dx - 1], {"sp": z * X + xo})

    def for_sends(dz, own, act):
        @pl.when(z < Z - 1)
        def _():
            for c in z_copies(dz):
                act(c)

        for dx in range(1, X):
            if own:

                @pl.when(lax.rem(x + dx, X) > x)
                def _():
                    for c in x_copies(dz, dx):
                        act(c)
            else:
                for c in x_copies(dz, dx):
                    act(c)

    def kv_wait(j):
        for c in block_copies(j, 0, zsend, {"sp": lax.rem(sp + X, SP)}):
            c.wait_recv()

    for_sends(0, True, lambda c: c.start())

    for k in range(1, TP):
        t = lax.rem(tp + k, TP)
        cols = pl.ds(pl.multiple_of(t * oc, 128), oc)
        for i, (w, buf) in enumerate(((out_lru, wl_buf), (out_fox, wf_buf))):
            s = remote(w.at[:, cols], buf.at[tp], wsend.at[i, k], wrecv.at[i, tp], {"tp": t})
            s.start()
            pending.append(s)

    gate_ref[...] = scaled(3)
    q_ref[...] = scaled(4)

    @pl.when(sp == 0)
    def _():
        pad[0:8, :] = jnp.zeros((8, lw), F32)

    @pl.when(sp > 0)
    def _():
        halo_copy.wait_recv()
        pad[0:8, :] = halo[...].astype(F32)[hb - 8 : hb, :]

    pad[8 : 8 + rows, :] = lru_ref[...].astype(F32)
    chans = pl.ds(pl.multiple_of(tp * lw, 128), lw)
    taps = conv_w.shape[0]
    taps_f32 = conv_w[:, chans].astype(F32)
    conv = jnp.zeros((rows, lw), F32)
    for j in range(taps):
        conv = conv + taps_f32[j : j + 1, :] * pad[8 - (taps - 1) + j : 8 - (taps - 1) + j + rows, :]
    conv_b = conv.astype(BF16)

    def sigmoid(v):
        return 1.0 / (1.0 + jnp.exp(-v))

    recur_gate = sigmoid(jnp.dot(conv_b, bd_r[...], preferred_element_type=F32))
    input_gate = sigmoid(jnp.dot(conv_b, bd_i[...], preferred_element_type=F32))
    own_rate = rate[:, chans]
    softplus = jnp.maximum(-own_rate, 0.0) + jnp.log1p(jnp.exp(-jnp.abs(own_rate)))
    for c in own_loads:
        c.wait()
    log_decay = -decay_sharpness * softplus * recur_gate + decay_buf[...]
    prefix_ref[...] = jnp.exp(log_decay)
    local_ref[...] = jnp.sqrt(one_minus_exp(2.0 * log_decay)) * input_gate * conv_b.astype(F32)
    row_id = lax.broadcasted_iota(jnp.int32, (rows, lw), 0)
    step = 1
    while step < rows:
        a = prefix_ref[...]
        b = local_ref[...]
        keep = row_id >= step
        a_prev = jnp.where(keep, pltpu.roll(a, step, 0), 1.0)
        b_prev = jnp.where(keep, pltpu.roll(b, step, 0), 0.0)
        local_ref[...] = b + a * b_prev
        prefix_ref[...] = a * a_prev
        step *= 2
    ends[sp, 0:1, :] = prefix_ref[rows - 1 : rows, :]
    ends[sp, 1:2, :] = local_ref[rows - 1 : rows, :]

    def end_copy(k):
        return remote(
            ends.at[sp], ends.at[sp], esend.at[k], erecv.at[sp], {"sp": lax.rem(sp + k, SP)}
        )

    for k in range(1, SP):

        @pl.when(sp + k < SP)
        def _():
            end_copy(k).start()

    score_scale = HEAD_DIM ** (-0.5)
    qc = rc

    def attend(j, diagonal):
        def some(i, carry):
            r = pl.ds(pl.multiple_of(i * qc, qc), qc)
            for h in range(H):
                hs = slice(h * HEAD_DIM, (h + 1) * HEAD_DIM)
                vs = slice(fw + h * HEAD_DIM, fw + (h + 1) * HEAD_DIM)
                s = lax.dot_general(
                    q_ref[r, hs],
                    kv_buf[j, :, hs],
                    (((1,), (1,)), ((), ())),
                    preferred_element_type=F32,
                )
                s = s * score_scale + forget[r, h : h + 1] - cum_buf[j, h : h + 1, :]
                if diagonal:
                    causal = (
                        lax.broadcasted_iota(jnp.int32, (qc, rows), 0) + i * qc
                        >= lax.broadcasted_iota(jnp.int32, (qc, rows), 1)
                    )
                    s = jnp.where(causal, s, -1e30)
                top = jnp.max(s, axis=1, keepdims=True)
                if diagonal:
                    p = jnp.exp(s - top)
                    m_ref[h, r, :] = top
                    l_ref[h, r, :] = jnp.sum(p, axis=1, keepdims=True)
                    o_ref[h, r, :] = jnp.dot(
                        p.astype(BF16), kv_buf[j, :, vs], preferred_element_type=F32
                    )
                else:
                    old = m_ref[h, r, :]
                    new = jnp.maximum(old, top)
                    p = jnp.exp(s - new)
                    fade = jnp.exp(old - new)
                    m_ref[h, r, :] = new
                    l_ref[h, r, :] = l_ref[h, r, :] * fade + jnp.sum(p, axis=1, keepdims=True)
                    o_ref[h, r, :] = o_ref[h, r, :] * fade + jnp.dot(
                        p.astype(BF16), kv_buf[j, :, vs], preferred_element_type=F32
                    )
            return carry

        lax.fori_loop(0, rows // qc, some, 0)

    attend(sp, True)

    def row_blocks(dz):
        for dx in range(1, X):
            xo = lax.rem(x + dx, X)

            @pl.when(jnp.logical_or(dz > 0, xo < x))
            def _():
                j = (z - dz) * X + xo
                kv_wait(j)
                attend(j, False)

    def finish_lru():
        incoming[...] = jnp.zeros_like(incoming)
        for j in range(SP - 1):

            @pl.when(j < sp)
            def _():
                remote(
                    ends.at[j], ends.at[j], esend.at[0], erecv.at[j], {"sp": lax.rem(sp + 1, SP)}
                ).wait_recv()
                incoming[...] = ends[j, 0:1, :] * incoming[...] + ends[j, 1:2, :]

        states = local_ref[...] + prefix_ref[...] * incoming[...]
        g = gate_ref[...].astype(F32)
        gelu = 0.5 * g * (1.0 + jnp.tanh(0.7978845608028654 * (g + 0.044715 * (g * g * g))))
        br_lru[tp] = (states * gelu).astype(BF16)
        for k in range(1, TP):
            lru_copy(k).start()

    def lru_copy(k):
        t = lax.rem(tp + k, TP)
        return remote(br_lru.at[tp], br_lru.at[tp], lsend.at[k], lrecv.at[tp], {"tp": t})

    lru_step = min(2, Z - 1)
    if Z == 1:
        finish_lru()

    def hop(dz, carry):
        @pl.when(dz <= z)
        def _():
            j = (z - dz) * X + x
            kv_wait(j)
            for_sends(dz, False, lambda c: c.start())
            row_blocks(dz - 1)
            attend(j, False)

        @pl.when(dz == lru_step)
        def _():
            finish_lru()

        return carry

    lax.fori_loop(1, Z, hop, 0)

    for k in range(TP):
        t = lax.rem(tp + k, TP)
        if k > 0:
            for i, buf in enumerate((wl_buf, wf_buf)):
                remote(buf.at[t], buf.at[t], wsend.at[i, k], wrecv.at[i, t], {"tp": t}).wait_recv()
            remote(br_lru.at[t], br_lru.at[t], lsend.at[k], lrecv.at[t], {"tp": t}).wait_recv()
        dot = jnp.dot(br_lru[t], wl_buf[t], preferred_element_type=F32)
        if k == 0:
            oacc[...] = dot
        else:
            oacc[...] += dot

    row_blocks(z)

    for c in range(CH):
        r = chunk(c)
        for h in range(H):
            br_fox[tp, r, h * HEAD_DIM : (h + 1) * HEAD_DIM] = (
                o_ref[h, r, :] / l_ref[h, r, :]
            ).astype(BF16)
        ref = br_fox.at[tp, r]
        for k in list(range(1, Y)) + [0]:
            to = far[k] if k else partner
            s = remote(ref, ref, fsend.at[k, c], frecv.at[tp, c], {"tp": to})
            s.start()
            pending.append(s)

    def fox_wait(src, c):
        ref = br_fox.at[src, chunk(c)]
        remote(ref, ref, fsend.at[0, c], frecv.at[src, c], {"tp": partner}).wait_recv()

    def fox_dot(src, r):
        return jnp.dot(br_fox[src, r, :], wf_buf[src], preferred_element_type=F32)

    for c in range(CH):
        fox_wait(partner, c)
        oacc[chunk(c), :] += fox_dot(tp, chunk(c)) + fox_dot(partner, chunk(c))
    for c in range(CH):
        r = chunk(c)
        for k in range(1, Y):
            fox_wait(far[k], c)
            ref = br_fox.at[far[k], r]
            s = remote(ref, ref, ffwd.at[k, c], frecv.at[far[k], c], {"tp": partner})
            s.start()
            pending.append(s)
            oacc[r, :] += fox_dot(far[k], r)
        for k in range(1, Y):
            fox_wait(pfar[k], c)
            oacc[r, :] += fox_dot(pfar[k], r)
        out[r, :] = oacc[r, :].astype(out.dtype)

    for s in pending:
        s.wait_send()
    for k in range(1, TP):
        lru_copy(k).wait_send()

    @pl.when(sp < SP - 1)
    def _():
        halo_copy.wait_send()

    for k in range(1, SP):

        @pl.when(sp + k < SP)
        def _():
            end_copy(k).wait_send()

    for_sends(0, True, lambda c: c.wait_send())

    def drain(dz, carry):
        @pl.when(dz <= z)
        def _():
            for_sends(dz, False, lambda c: c.wait_send())

        return carry

    lax.fori_loop(1, Z, drain, 0)


def shards(SP, TP, X, *args):
    tokens, lru_in, gate_in, query_w = args[:4]
    (conv_weight, rg_w, ig_w, rate, decay_extra, forget, out_lru, out_fox) = args[6:]
    rows, dcols = tokens.shape
    D, lw = lru_in.shape
    fw = query_w.shape[1]
    oc = out_lru.shape[1] // TP
    tot = 2 * lw + 3 * fw
    H = fw // HEAD_DIM
    Y = TP // 2
    Z = SP // X
    CH = 2
    vm = pl.BlockSpec(memory_space=pltpu.VMEM)
    hbm = pl.BlockSpec(memory_space=pl.ANY)
    dma = pltpu.SemaphoreType.DMA
    V = pltpu.VMEM
    scratch = [
        V((TP, rows, dcols), BF16),
        V((D, tot), BF16),
        V((rows, tot), F32),
        V((rows, 1), F32),
        V((rows, lw), BF16),
        V((16, lw), BF16),
        V((rows + 8, lw), F32),
        V((lw, lw), BF16),
        V((lw, lw), BF16),
        V((rows, lw), BF16),
        V((rows, fw), BF16),
        V((rows, lw), F32),
        V((rows, lw), F32),
        V((rows, lw), F32),
        V((SP, 8, lw), F32),
        V((1, lw), F32),
        V((SP, rows, 2 * fw), BF16),
        V((SP, 8, rows), F32),
        V((rows, 128), F32),
        V((H, rows, 1), F32),
        V((H, rows, 1), F32),
        V((H, rows, HEAD_DIM), F32),
        V((TP, lw, oc), BF16),
        V((TP, fw, oc), BF16),
        V((TP, rows, lw), BF16),
        V((TP, rows, fw), BF16),
        V((rows, oc), F32),
        dma((8,)),
        dma((Y, CH)),
        dma((Y, CH)),
        dma((TP, CH)),
        dma((1,)),
        dma((1,)),
        dma((SP,)),
        dma((SP,)),
        dma((Z, 2)),
        dma((max(X - 1, 1), Z, 2)),
        dma((SP, 2)),
        dma((2, TP)),
        dma((2, TP)),
        dma((TP,)),
        dma((TP,)),
        dma((Y, CH)),
        dma((Y, CH)),
        dma((TP, CH)),
    ]
    return pl.pallas_call(
        functools.partial(kernel, SP, TP, X),
        out_shape=jax.ShapeDtypeStruct((rows, oc), BF16),
        in_specs=[vm] + [hbm] * 5 + [vm] * 4 + [hbm, vm, hbm, hbm],
        out_specs=vm,
        scratch_shapes=scratch,
        compiler_params=pltpu.CompilerParams(
            collective_id=0, has_side_effects=True, vmem_limit_bytes=60 * 1024 * 1024
        ),
    )(*args[:9], rate.reshape(1, -1), decay_extra, forget, out_lru, out_fox)


def columns_of(mesh):
    SP = mesh.shape["sp"]
    try:
        X = len({d.coords[0] for d in mesh.devices.flat})
    except AttributeError:
        X = 2
    return X if SP % X == 0 else 1


def solution(mesh):
    placed = (
        P("sp", "tp"),
        P(None, "tp"),
        P(None, "tp"),
        P(None, "tp"),
        P(None, "tp"),
        P(None, "tp"),
        P(),
        P(),
        P(),
        P(),
        P("sp", "tp"),
        P("sp", "tp"),
        P("tp", None),
        P("tp", None),
    )
    body = functools.partial(shards, mesh.shape["sp"], mesh.shape["tp"], columns_of(mesh))
    return jax.shard_map(
        body, mesh=mesh, in_specs=placed, out_specs=P("sp", "tp"), check_vma=False
    )
```

```python
import functools

import jax
import jax.numpy as jnp
from jax import lax
from jax.experimental import pallas as pl
from jax.experimental.pallas import tpu as pltpu
from jax.sharding import PartitionSpec as P

HEAD_DIM = 128
decay_sharpness = 8.0
epsilon_norm = 1e-06
MESH = pl.DeviceIdType.MESH
F32 = jnp.float32
BF16 = jnp.bfloat16


def one_minus_exp(w):
    u = -w
    series = 1.0 - u / 9.0
    for n in range(8, 1, -1):
        series = 1.0 - u / n * series
    return jnp.where(u < 0.5, u * series, 1.0 - jnp.exp(w))


def remote(src, dst, send_sem, recv_sem, device):
    return pltpu.make_async_remote_copy(
        src_ref=src,
        dst_ref=dst,
        send_sem=send_sem,
        recv_sem=recv_sem,
        device_id=device,
        device_id_type=MESH,
    )


def kernel(
    SP,
    TP,
    X,
    tokens,
    lru_in,
    gate_in,
    query_w,
    key_w,
    value_w,
    conv_w,
    rg_w,
    ig_w,
    rate,
    decay_extra,
    forget,
    out_lru,
    out_fox,
    out,
    tok_buf,
    w_buf,
    acc,
    sq,
    lru_ref,
    halo,
    pad,
    bd_r,
    bd_i,
    gate_ref,
    q_ref,
    decay_buf,
    prefix_ref,
    local_ref,
    ends,
    incoming,
    kv_buf,
    cum_buf,
    cum_pad,
    wide,
    fcol,
    m_ref,
    l_ref,
    o_ref,
    q_far,
    m_far,
    l_far,
    o_far,
    part_out,
    stat_out,
    part_in,
    stat_in,
    wl_buf,
    wf_buf,
    br_lru,
    br_fox,
    oacc,
    load_sem,
    tsend,
    tfwd,
    trecv,
    hsend,
    hrecv,
    esend,
    erecv,
    zsend,
    xsend,
    kvrecv,
    wsend,
    wrecv,
    lsend,
    lrecv,
    fsend,
    ffwd,
    frecv,
    lfwd,
    qsend,
    qrecv,
    osend,
    orecv,
):
    rows, dcols = tokens.shape
    D, lw = lru_in.shape
    fw = query_w.shape[1]
    H = fw // HEAD_DIM
    oc = out.shape[1]
    Y = TP // 2
    Z = SP // X
    CH = tsend.shape[1]
    rc = rows // CH
    sp = lax.axis_index("sp")
    tp = lax.axis_index("tp")
    z = lax.div(sp, X)
    x = lax.rem(sp, X)
    partner = tp + 1 - 2 * lax.rem(tp, 2)
    far = [lax.rem(tp + 2 * k, TP) for k in range(Y)]
    pfar = [lax.rem(partner + 2 * k, TP) for k in range(Y)]
    offs = [0, lw, lw + fw, lw + 2 * fw, 2 * lw + 2 * fw, 2 * lw + 3 * fw]

    barrier = pltpu.get_barrier_semaphore()
    for k in range(1, SP):
        pl.semaphore_signal(
            barrier, inc=1, device_id={"sp": lax.rem(sp + k, SP)}, device_id_type=MESH
        )
    for k in range(1, TP):
        pl.semaphore_signal(
            barrier, inc=1, device_id={"tp": lax.rem(tp + k, TP)}, device_id_type=MESH
        )
    loads = []
    for i, w in enumerate((lru_in, key_w, value_w, gate_in, query_w)):
        c = pltpu.make_async_copy(w, w_buf.at[:, offs[i] : offs[i + 1]], load_sem.at[i])
        c.start()
        loads.append(c)
    mine = pl.ds(pl.multiple_of(tp * oc, 128), oc)
    own_loads = [
        pltpu.make_async_copy(decay_extra, decay_buf, load_sem.at[5]),
        pltpu.make_async_copy(out_lru.at[:, mine], wl_buf.at[tp], load_sem.at[6]),
        pltpu.make_async_copy(out_fox.at[:, mine], wf_buf.at[tp], load_sem.at[7]),
    ]
    for c in own_loads:
        c.start()
    pl.semaphore_wait(barrier, SP - 1 + TP - 1)

    pending = []

    def chunk(c):
        return pl.ds(c * rc, rc)

    for c in range(CH):
        for k in range(1, Y):
            s = remote(
                tokens.at[chunk(c)],
                tok_buf.at[tp, chunk(c)],
                tsend.at[k, c],
                trecv.at[tp, c],
                {"tp": far[k]},
            )
            s.start()
            pending.append(s)
    for c in range(CH):
        s = remote(
            tokens.at[chunk(c)],
            tok_buf.at[tp, chunk(c)],
            tsend.at[0, c],
            trecv.at[tp, c],
            {"tp": partner},
        )
        s.start()
        pending.append(s)

    bw = rg_w.shape[1]
    nb = lw // bw
    bd_r[...] = jnp.zeros_like(bd_r)
    bd_i[...] = jnp.zeros_like(bd_i)
    for n in range(nb):
        sl = pl.ds(n * bw, bw)
        bd_r[sl, sl] = rg_w[tp * nb + n]
        bd_i[sl, sl] = ig_w[tp * nb + n]
    cum_pad[...] = jnp.zeros_like(cum_pad)
    wide[...] = jnp.zeros_like(wide)
    wide[0:H, :] = forget[...]
    fcol[...] = wide[...].T
    cum_buf[sp] = wide[0:8, :]

    for c in loads:
        c.wait()

    def project(val, src, r, first=False):
        w_rows = pl.ds(pl.multiple_of(src * dcols, dcols), dcols)
        v32 = val.astype(F32)
        part = jnp.sum(v32 * v32, axis=1, keepdims=True)
        dot = jnp.dot(val, w_buf[w_rows, :], preferred_element_type=F32)
        if first:
            sq[r, :] = part
            acc[r, :] = dot
        else:
            sq[r, :] += part
            acc[r, :] += dot

    def tok_wait(src, c):
        ref = tok_buf.at[src, chunk(c)]
        remote(ref, ref, tsend.at[0, c], trecv.at[src, c], {"tp": partner}).wait_recv()

    for c in range(CH):
        project(tokens[chunk(c), :], tp, chunk(c), True)
    for c in range(CH):
        tok_wait(partner, c)
        project(tok_buf[partner, chunk(c), :], partner, chunk(c))
    for c in range(CH):
        for k in range(1, Y):
            tok_wait(far[k], c)
            ref = tok_buf.at[far[k], chunk(c)]
            s = remote(ref, ref, tfwd.at[k, c], trecv.at[far[k], c], {"tp": partner})
            s.start()
            pending.append(s)
            project(tok_buf[far[k], chunk(c), :], far[k], chunk(c))
        for k in range(1, Y):
            tok_wait(pfar[k], c)
            project(tok_buf[pfar[k], chunk(c), :], pfar[k], chunk(c))

    row_scale = lax.rsqrt(sq[...] / D + epsilon_norm)

    def scaled(i, n=1):
        return (acc[:, offs[i] : offs[i + n]] * row_scale).astype(BF16)

    lru_ref[...] = scaled(0)
    hb = halo.shape[0]
    halo_copy = remote(
        lru_ref.at[pl.ds(rows - hb, hb)],
        halo,
        hsend.at[0],
        hrecv.at[0],
        {"sp": lax.rem(sp + 1, SP)},
    )

    @pl.when(sp < SP - 1)
    def _():
        halo_copy.start()

    kv_buf[sp] = scaled(1, 2)

    paired = Z in (3, 4)
    helper = jnp.logical_and(z <= Z - 3, paired)
    helped = jnp.logical_and(z >= 2, paired)

    def block_copies(j, a, send_sem, device):
        return (
            remote(kv_buf.at[j], kv_buf.at[j], send_sem.at[a, 0], kvrecv.at[j, 0], device),
            remote(cum_buf.at[j], cum_buf.at[j], send_sem.at[a, 1], kvrecv.at[j, 1], device),
        )

    def z_copies(dz):
        j = (z - dz) * X + x
        return block_copies(j, dz, zsend, {"sp": lax.rem(sp + X, SP)})

    def x_copies(dz, dx):
        j = (z - dz) * X + x
        xo = lax.rem(x + dx, X)
        return block_copies(j, dz, xsend.at[dx - 1], {"sp": z * X + xo})

    def for_sends(dz, own, act):
        if own or not paired:

            @pl.when(z < Z - 1)
            def _():
                for c in z_copies(dz):
                    act(c)

        for dx in range(1, X):
            if own:

                @pl.when(jnp.logical_or(lax.rem(x + dx, X) > x, helper))
                def _():
                    for c in x_copies(dz, dx):
                        act(c)
            else:
                for c in x_copies(dz, dx):
                    act(c)

    def kv_wait(j):
        for c in block_copies(j, 0, zsend, {"sp": lax.rem(sp + X, SP)}):
            c.wait_recv()

    for_sends(0, True, lambda c: c.start())

    q_ref[...] = scaled(4)
    q_copy = remote(
        q_ref, q_far, qsend.at[0], qrecv.at[0], {"sp": lax.rem(sp + SP - 2 * X, SP)}
    )

    @pl.when(helped)
    def _():
        q_copy.start()

    for i, (w, buf) in enumerate(((out_lru, wl_buf), (out_fox, wf_buf))):
        for k in range(1, TP):
            t = lax.rem(tp + k, TP)
            cols = pl.ds(pl.multiple_of(t * oc, 128), oc)
            s = remote(w.at[:, cols], buf.at[tp], wsend.at[i, k], wrecv.at[i, tp], {"tp": t})
            s.start()
            pending.append(s)

    gate_ref[...] = scaled(3)

    @pl.when(sp == 0)
    def _():
        pad[0:8, :] = jnp.zeros((8, lw), F32)

    @pl.when(sp > 0)
    def _():
        halo_copy.wait_recv()
        pad[0:8, :] = halo[...].astype(F32)[hb - 8 : hb, :]

    pad[8 : 8 + rows, :] = lru_ref[...].astype(F32)
    chans = pl.ds(pl.multiple_of(tp * lw, 128), lw)
    taps = conv_w.shape[0]
    taps_f32 = conv_w[:, chans].astype(F32)
    conv = jnp.zeros((rows, lw), F32)
    for j in range(taps):
        conv = conv + taps_f32[j : j + 1, :] * pad[8 - (taps - 1) + j : 8 - (taps - 1) + j + rows, :]
    conv_b = conv.astype(BF16)

    def sigmoid(v):
        return 1.0 / (1.0 + jnp.exp(-v))

    recur_gate = sigmoid(jnp.dot(conv_b, bd_r[...], preferred_element_type=F32))
    input_gate = sigmoid(jnp.dot(conv_b, bd_i[...], preferred_element_type=F32))
    own_rate = rate[:, chans]
    softplus = jnp.maximum(-own_rate, 0.0) + jnp.log1p(jnp.exp(-jnp.abs(own_rate)))
    for c in own_loads:
        c.wait()
    log_decay = -decay_sharpness * softplus * recur_gate + decay_buf[...]
    prefix_ref[...] = jnp.exp(log_decay)
    local_ref[...] = jnp.sqrt(one_minus_exp(2.0 * log_decay)) * input_gate * conv_b.astype(F32)
    row_id = lax.broadcasted_iota(jnp.int32, (rows, lw), 0)
    step = 1
    while step < rows:
        a = prefix_ref[...]
        b = local_ref[...]
        keep = row_id >= step
        a_prev = jnp.where(keep, pltpu.roll(a, step, 0), 1.0)
        b_prev = jnp.where(keep, pltpu.roll(b, step, 0), 0.0)
        local_ref[...] = b + a * b_prev
        prefix_ref[...] = a * a_prev
        step *= 2
    ends[sp, 0:1, :] = prefix_ref[rows - 1 : rows, :]
    ends[sp, 1:2, :] = local_ref[rows - 1 : rows, :]

    def end_copy(k):
        return remote(
            ends.at[sp], ends.at[sp], esend.at[k], erecv.at[sp], {"sp": lax.rem(sp + k, SP)}
        )

    for k in range(1, SP):

        @pl.when(sp + k < SP)
        def _():
            end_copy(k).start()

    score_scale = HEAD_DIM ** (-0.5)
    qc = rc

    def attend(j, diagonal, far_first=None):
        other = far_first is not None
        first = diagonal or far_first
        qs, ms, ls, os = (q_far, m_far, l_far, o_far) if other else (q_ref, m_ref, l_ref, o_ref)

        def some(i, carry):
            r = pl.ds(pl.multiple_of(i * qc, qc), qc)
            for h in range(H):
                hs = slice(h * HEAD_DIM, (h + 1) * HEAD_DIM)
                vs = slice(fw + h * HEAD_DIM, fw + (h + 1) * HEAD_DIM)
                s = lax.dot_general(
                    qs[r, hs],
                    kv_buf[j, :, hs],
                    (((1,), (1,)), ((), ())),
                    preferred_element_type=F32,
                )
                s = s * score_scale
                if not other:
                    s = s + fcol[r, h : h + 1]
                s = s - cum_buf[j, h : h + 1, :]
                if diagonal:
                    causal = (
                        lax.broadcasted_iota(jnp.int32, (qc, rows), 0) + i * qc
                        >= lax.broadcasted_iota(jnp.int32, (qc, rows), 1)
                    )
                    s = jnp.where(causal, s, -1e30)
                top = jnp.max(s, axis=1, keepdims=True)
                if first:
                    p = jnp.exp(s - top)
                    ms[h, r, :] = top
                    ls[h, r, :] = jnp.sum(p, axis=1, keepdims=True)
                    os[h, r, :] = jnp.dot(
                        p.astype(BF16), kv_buf[j, :, vs], preferred_element_type=F32
                    )
                else:
                    old = ms[h, r, :]
                    new = jnp.maximum(old, top)
                    p = jnp.exp(s - new)
                    fade = jnp.exp(old - new)
                    ms[h, r, :] = new
                    ls[h, r, :] = ls[h, r, :] * fade + jnp.sum(p, axis=1, keepdims=True)
                    os[h, r, :] = os[h, r, :] * fade + jnp.dot(
                        p.astype(BF16), kv_buf[j, :, vs], preferred_element_type=F32
                    )
            return carry

        lax.fori_loop(0, rows // qc, some, 0)

    attend(sp, True)

    def row_blocks(dz):
        for dx in range(1, X):
            xo = lax.rem(x + dx, X)

            @pl.when(jnp.logical_or(dz > 0, xo < x))
            def _():
                j = (z - dz) * X + xo
                kv_wait(j)
                attend(j, False)

    def finish_lru():
        incoming[...] = jnp.zeros_like(incoming)
        for j in range(SP - 1):

            @pl.when(j < sp)
            def _():
                remote(
                    ends.at[j], ends.at[j], esend.at[0], erecv.at[j], {"sp": lax.rem(sp + 1, SP)}
                ).wait_recv()
                incoming[...] = ends[j, 0:1, :] * incoming[...] + ends[j, 1:2, :]

        states = local_ref[...] + prefix_ref[...] * incoming[...]
        g = gate_ref[...].astype(F32)
        gelu = 0.5 * g * (1.0 + jnp.tanh(0.7978845608028654 * (g + 0.044715 * (g * g * g))))
        br_lru[tp] = (states * gelu).astype(BF16)
        for k in range(Y - 1, -1, -1):
            lru_copy(k).start()

    def lru_copy(k):
        to = far[k] if k else partner
        return remote(br_lru.at[tp], br_lru.at[tp], lsend.at[k], lrecv.at[tp], {"tp": to})

    lru_step = min(2, Z - 1)
    if Z == 1:
        finish_lru()

    def hop(dz, carry):
        @pl.when(dz <= z)
        def _():
            j = (z - dz) * X + x
            kv_wait(j)
            for_sends(dz, False, lambda c: c.start())
            row_blocks(dz - 1)
            attend(j, False)

        @pl.when(dz == lru_step)
        def _():
            finish_lru()

        return carry

    up = {"sp": lax.rem(sp + 2 * X, SP)}
    part_copies = (
        remote(part_out, part_in, osend.at[0], orecv.at[0], up),
        remote(stat_out, stat_in, osend.at[1], orecv.at[1], up),
    )

    def send_partial():
        for h in range(H):
            part_out[:, h * HEAD_DIM : (h + 1) * HEAD_DIM] = o_far[h].astype(BF16)
            cum_pad[:, h : h + 1] = m_far[h]
            cum_pad[:, H + h : H + h + 1] = l_far[h]
        stat_out[...] = cum_pad[...].T[0:8, :]
        for c in part_copies:
            c.start()

    if paired:
        below = (z - 1) * X

        @pl.when(helper)
        def _():
            q_copy.wait_recv()
            attend(sp, False, True)

        @pl.when(z >= 1)
        def _():
            kv_wait(below + x)
            for_sends(1, False, lambda c: c.start())

        for dx in range(1, X):
            xo = lax.rem(x + dx, X)

            @pl.when(jnp.logical_or(xo < x, helper))
            def _():
                kv_wait(z * X + xo)

            @pl.when(helper)
            def _():
                attend(z * X + xo, False, False)

        @pl.when(jnp.logical_and(helper, z == 0))
        def _():
            send_partial()

        for dx in range(1, X):
            xo = lax.rem(x + dx, X)

            @pl.when(xo < x)
            def _():
                attend(z * X + xo, False)

        finish_lru()

        @pl.when(jnp.logical_and(helper, z >= 1))
        def _():
            attend(below + x, False, False)

        @pl.when(z >= 1)
        def _():
            attend(below + x, False)
            for dx in range(1, X):
                j = below + lax.rem(x + dx, X)
                kv_wait(j)

                @pl.when(helper)
                def _():
                    attend(j, False, False)

            @pl.when(helper)
            def _():
                send_partial()

            for dx in range(1, X):
                attend(below + lax.rem(x + dx, X), False)

    else:
        lax.fori_loop(1, Z, hop, 0)

    def lru_wait(t):
        remote(br_lru.at[t], br_lru.at[t], lsend.at[0], lrecv.at[t], {"tp": partner}).wait_recv()

    def lru_dot(t):
        return jnp.dot(br_lru[t], wl_buf[t], preferred_element_type=F32)

    oacc[...] = lru_dot(tp)
    for k in range(1, TP):
        t = lax.rem(tp + k, TP)
        for i, buf in enumerate((wl_buf, wf_buf)):
            remote(buf.at[t], buf.at[t], wsend.at[i, k], wrecv.at[i, t], {"tp": t}).wait_recv()
    for k in range(1, Y):
        lru_wait(far[k])
        ref = br_lru.at[far[k]]
        s = remote(ref, ref, lfwd.at[k], lrecv.at[far[k]], {"tp": partner})
        s.start()
        pending.append(s)
    lru_wait(partner)
    oacc[...] += lru_dot(partner)
    for k in range(1, Y):
        oacc[...] += lru_dot(far[k])
        lru_wait(pfar[k])
        oacc[...] += lru_dot(pfar[k])

    if paired:

        @pl.when(helped)
        def _():
            for c in part_copies:
                c.wait_recv()
            wide[0:8, :] = stat_in[...]
            stats = wide[...].T
            for h in range(H):
                m_in = stats[:, h : h + 1] + fcol[:, h : h + 1]
                l_in = stats[:, H + h : H + h + 1]
                part = part_in[:, h * HEAD_DIM : (h + 1) * HEAD_DIM].astype(F32)
                new = jnp.maximum(m_ref[h], m_in)
                fade = jnp.exp(m_ref[h] - new)
                grow = jnp.exp(m_in - new)
                l_ref[h] = l_ref[h] * fade + l_in * grow
                o_ref[h] = o_ref[h] * fade + part * grow

    else:
        row_blocks(z)

    for c in range(CH):
        r = chunk(c)
        for h in range(H):
            br_fox[tp, r, h * HEAD_DIM : (h + 1) * HEAD_DIM] = (
                o_ref[h, r, :] / l_ref[h, r, :]
            ).astype(BF16)
        ref = br_fox.at[tp, r]
        for k in list(range(1, Y)) + [0]:
            to = far[k] if k else partner
            s = remote(ref, ref, fsend.at[k, c], frecv.at[tp, c], {"tp": to})
            s.start()
            pending.append(s)

    def fox_wait(src, c):
        ref = br_fox.at[src, chunk(c)]
        remote(ref, ref, fsend.at[0, c], frecv.at[src, c], {"tp": partner}).wait_recv()

    def fox_dot(src, r):
        return jnp.dot(br_fox[src, r, :], wf_buf[src], preferred_element_type=F32)

    for c in range(CH):
        fox_wait(partner, c)
        oacc[chunk(c), :] += fox_dot(tp, chunk(c)) + fox_dot(partner, chunk(c))
    for c in range(CH):
        r = chunk(c)
        for k in range(1, Y):
            fox_wait(far[k], c)
            ref = br_fox.at[far[k], r]
            s = remote(ref, ref, ffwd.at[k, c], frecv.at[far[k], c], {"tp": partner})
            s.start()
            pending.append(s)
            oacc[r, :] += fox_dot(far[k], r)
        for k in range(1, Y):
            fox_wait(pfar[k], c)
            oacc[r, :] += fox_dot(pfar[k], r)
        out[r, :] = oacc[r, :].astype(out.dtype)

    for s in pending:
        s.wait_send()
    for k in range(Y):
        lru_copy(k).wait_send()

    @pl.when(helped)
    def _():
        q_copy.wait_send()

    @pl.when(helper)
    def _():
        for c in part_copies:
            c.wait_send()

    @pl.when(sp < SP - 1)
    def _():
        halo_copy.wait_send()

    for k in range(1, SP):

        @pl.when(sp + k < SP)
        def _():
            end_copy(k).wait_send()

    for_sends(0, True, lambda c: c.wait_send())

    def drain(dz, carry):
        @pl.when(dz <= z)
        def _():
            for_sends(dz, False, lambda c: c.wait_send())

        return carry

    if paired:

        @pl.when(z >= 1)
        def _():
            for_sends(1, False, lambda c: c.wait_send())

    else:
        lax.fori_loop(1, Z, drain, 0)


def shards(SP, TP, X, *args):
    tokens, lru_in, gate_in, query_w = args[:4]
    (conv_weight, rg_w, ig_w, rate, decay_extra, forget, out_lru, out_fox) = args[6:]
    rows, dcols = tokens.shape
    D, lw = lru_in.shape
    fw = query_w.shape[1]
    oc = out_lru.shape[1] // TP
    tot = 2 * lw + 3 * fw
    H = fw // HEAD_DIM
    Y = TP // 2
    Z = SP // X
    CH = 2
    vm = pl.BlockSpec(memory_space=pltpu.VMEM)
    hbm = pl.BlockSpec(memory_space=pl.ANY)
    dma = pltpu.SemaphoreType.DMA
    V = pltpu.VMEM
    scratch = [
        V((TP, rows, dcols), BF16),
        V((D, tot), BF16),
        V((rows, tot), F32),
        V((rows, 1), F32),
        V((rows, lw), BF16),
        V((16, lw), BF16),
        V((rows + 8, lw), F32),
        V((lw, lw), BF16),
        V((lw, lw), BF16),
        V((rows, lw), BF16),
        V((rows, fw), BF16),
        V((rows, lw), F32),
        V((rows, lw), F32),
        V((rows, lw), F32),
        V((SP, 8, lw), F32),
        V((1, lw), F32),
        V((SP, rows, 2 * fw), BF16),
        V((SP, 8, rows), F32),
        V((rows, 128), F32),
        V((128, rows), F32),
        V((rows, 128), F32),
        V((H, rows, 1), F32),
        V((H, rows, 1), F32),
        V((H, rows, HEAD_DIM), F32),
        V((rows, fw), BF16),
        V((H, rows, 1), F32),
        V((H, rows, 1), F32),
        V((H, rows, HEAD_DIM), F32),
        V((rows, fw), BF16),
        V((8, rows), F32),
        V((rows, fw), BF16),
        V((8, rows), F32),
        V((TP, lw, oc), BF16),
        V((TP, fw, oc), BF16),
        V((TP, rows, lw), BF16),
        V((TP, rows, fw), BF16),
        V((rows, oc), F32),
        dma((8,)),
        dma((Y, CH)),
        dma((Y, CH)),
        dma((TP, CH)),
        dma((1,)),
        dma((1,)),
        dma((SP,)),
        dma((SP,)),
        dma((Z, 2)),
        dma((max(X - 1, 1), Z, 2)),
        dma((SP, 2)),
        dma((2, TP)),
        dma((2, TP)),
        dma((TP,)),
        dma((TP,)),
        dma((Y, CH)),
        dma((Y, CH)),
        dma((TP, CH)),
        dma((Y,)),
        dma((1,)),
        dma((1,)),
        dma((2,)),
        dma((2,)),
    ]
    return pl.pallas_call(
        functools.partial(kernel, SP, TP, X),
        out_shape=jax.ShapeDtypeStruct((rows, oc), BF16),
        in_specs=[vm] + [hbm] * 5 + [vm] * 4 + [hbm, vm, hbm, hbm],
        out_specs=vm,
        scratch_shapes=scratch,
        compiler_params=pltpu.CompilerParams(
            collective_id=0, has_side_effects=True, vmem_limit_bytes=60 * 1024 * 1024
        ),
    )(*args[:9], rate.reshape(1, -1), decay_extra, forget.T, out_lru, out_fox)


def columns_of(mesh):
    SP = mesh.shape["sp"]
    try:
        X = len({d.coords[0] for d in mesh.devices.flat})
    except AttributeError:
        X = 2
    return X if SP % X == 0 else 1


def solution(mesh):
    placed = (
        P("sp", "tp"),
        P(None, "tp"),
        P(None, "tp"),
        P(None, "tp"),
        P(None, "tp"),
        P(None, "tp"),
        P(),
        P(),
        P(),
        P(),
        P("sp", "tp"),
        P("sp", "tp"),
        P("tp", None),
        P("tp", None),
    )
    body = functools.partial(shards, mesh.shape["sp"], mesh.shape["tp"], columns_of(mesh))
    return jax.shard_map(
        body, mesh=mesh, in_specs=placed, out_specs=P("sp", "tp"), check_vma=False
    )
```

```python
import functools

import jax
import jax.numpy as jnp
from jax import lax
from jax.experimental import pallas as pl
from jax.experimental.pallas import tpu as pltpu
from jax.sharding import PartitionSpec as P

HEAD_DIM = 128
decay_sharpness = 8.0
epsilon_norm = 1e-06
MESH = pl.DeviceIdType.MESH
F32 = jnp.float32
BF16 = jnp.bfloat16


def one_minus_exp(w):
    u = -w
    series = 1.0 - u / 9.0
    for n in range(8, 1, -1):
        series = 1.0 - u / n * series
    return jnp.where(u < 0.5, u * series, 1.0 - jnp.exp(w))


def remote(src, dst, send_sem, recv_sem, device):
    return pltpu.make_async_remote_copy(
        src_ref=src,
        dst_ref=dst,
        send_sem=send_sem,
        recv_sem=recv_sem,
        device_id=device,
        device_id_type=MESH,
    )


def kernel(
    SP,
    TP,
    X,
    tokens,
    lru_in,
    gate_in,
    query_w,
    key_w,
    value_w,
    conv_w,
    rg_w,
    ig_w,
    rate,
    decay_extra,
    forget,
    out_lru,
    out_fox,
    out,
    tok_buf,
    w_buf,
    acc,
    sq,
    lru_ref,
    halo,
    pad,
    bd_r,
    bd_i,
    gate_ref,
    q_ref,
    decay_buf,
    prefix_ref,
    local_ref,
    ends,
    incoming,
    kv_buf,
    cum_buf,
    cum_pad,
    wide,
    fcol,
    m_ref,
    l_ref,
    o_ref,
    q_far,
    m_far,
    l_far,
    o_far,
    part_out,
    stat_out,
    part_in,
    stat_in,
    wl_buf,
    wf_buf,
    br_lru,
    br_fox,
    oacc,
    load_sem,
    tsend,
    tfwd,
    trecv,
    hsend,
    hrecv,
    esend,
    erecv,
    zsend,
    xsend,
    kvrecv,
    wsend,
    wrecv,
    lsend,
    lrecv,
    fsend,
    ffwd,
    frecv,
    lfwd,
    qsend,
    qrecv,
    osend,
    orecv,
):
    rows, dcols = tokens.shape
    D, lw = lru_in.shape
    fw = query_w.shape[1]
    H = fw // HEAD_DIM
    oc = out.shape[1]
    Y = TP // 2
    Z = SP // X
    CH = tsend.shape[1]
    rc = rows // CH
    sp = lax.axis_index("sp")
    tp = lax.axis_index("tp")
    z = lax.div(sp, X)
    x = lax.rem(sp, X)
    partner = tp + 1 - 2 * lax.rem(tp, 2)
    far = [lax.rem(tp + 2 * k, TP) for k in range(Y)]
    pfar = [lax.rem(partner + 2 * k, TP) for k in range(Y)]
    offs = [0, lw, lw + fw, lw + 2 * fw, 2 * lw + 2 * fw, 2 * lw + 3 * fw]

    barrier = pltpu.get_barrier_semaphore()
    for k in range(1, SP):
        pl.semaphore_signal(
            barrier, inc=1, device_id={"sp": lax.rem(sp + k, SP)}, device_id_type=MESH
        )
    for k in range(1, TP):
        pl.semaphore_signal(
            barrier, inc=1, device_id={"tp": lax.rem(tp + k, TP)}, device_id_type=MESH
        )
    loads = []
    for i, w in enumerate((lru_in, key_w, value_w, gate_in, query_w)):
        c = pltpu.make_async_copy(w, w_buf.at[:, offs[i] : offs[i + 1]], load_sem.at[i])
        c.start()
        loads.append(c)
    mine = pl.ds(pl.multiple_of(tp * oc, 128), oc)
    own_loads = [
        pltpu.make_async_copy(decay_extra, decay_buf, load_sem.at[5]),
        pltpu.make_async_copy(out_lru.at[:, mine], wl_buf.at[tp], load_sem.at[6]),
        pltpu.make_async_copy(out_fox.at[:, mine], wf_buf.at[tp], load_sem.at[7]),
    ]
    for c in own_loads:
        c.start()
    pl.semaphore_wait(barrier, SP - 1 + TP - 1)

    pending = []

    def chunk(c):
        return pl.ds(c * rc, rc)

    for c in range(CH):
        for k in range(1, Y):
            s = remote(
                tokens.at[chunk(c)],
                tok_buf.at[tp, chunk(c)],
                tsend.at[k, c],
                trecv.at[tp, c],
                {"tp": far[k]},
            )
            s.start()
            pending.append(s)
    for c in range(CH):
        s = remote(
            tokens.at[chunk(c)],
            tok_buf.at[tp, chunk(c)],
            tsend.at[0, c],
            trecv.at[tp, c],
            {"tp": partner},
        )
        s.start()
        pending.append(s)

    bw = rg_w.shape[1]
    nb = lw // bw
    bd_r[...] = jnp.zeros_like(bd_r)
    bd_i[...] = jnp.zeros_like(bd_i)
    for n in range(nb):
        sl = pl.ds(n * bw, bw)
        bd_r[sl, sl] = rg_w[tp * nb + n]
        bd_i[sl, sl] = ig_w[tp * nb + n]
    cum_pad[...] = jnp.zeros_like(cum_pad)
    wide[...] = jnp.zeros_like(wide)
    wide[0:H, :] = forget[...]
    fcol[...] = wide[...].T
    cum_buf[sp] = wide[0:8, :]

    for c in loads:
        c.wait()

    def project(val, src, r, first=False):
        w_rows = pl.ds(pl.multiple_of(src * dcols, dcols), dcols)
        v32 = val.astype(F32)
        part = jnp.sum(v32 * v32, axis=1, keepdims=True)
        dot = jnp.dot(val, w_buf[w_rows, :], preferred_element_type=F32)
        if first:
            sq[r, :] = part
            acc[r, :] = dot
        else:
            sq[r, :] += part
            acc[r, :] += dot

    def tok_wait(src, c):
        ref = tok_buf.at[src, chunk(c)]
        remote(ref, ref, tsend.at[0, c], trecv.at[src, c], {"tp": partner}).wait_recv()

    for c in range(CH):
        project(tokens[chunk(c), :], tp, chunk(c), True)
    for c in range(CH):
        tok_wait(partner, c)
        project(tok_buf[partner, chunk(c), :], partner, chunk(c))
    for c in range(CH):
        for k in range(1, Y):
            tok_wait(far[k], c)
            ref = tok_buf.at[far[k], chunk(c)]
            s = remote(ref, ref, tfwd.at[k, c], trecv.at[far[k], c], {"tp": partner})
            s.start()
            pending.append(s)
            project(tok_buf[far[k], chunk(c), :], far[k], chunk(c))
        for k in range(1, Y):
            tok_wait(pfar[k], c)
            project(tok_buf[pfar[k], chunk(c), :], pfar[k], chunk(c))

    row_scale = lax.rsqrt(sq[...] / D + epsilon_norm)

    def scaled(i, n=1):
        return (acc[:, offs[i] : offs[i + n]] * row_scale).astype(BF16)

    lru_ref[...] = scaled(0)
    hb = halo.shape[0]
    halo_copy = remote(
        lru_ref.at[pl.ds(rows - hb, hb)],
        halo,
        hsend.at[0],
        hrecv.at[0],
        {"sp": lax.rem(sp + 1, SP)},
    )

    @pl.when(sp < SP - 1)
    def _():
        halo_copy.start()

    kv_buf[sp] = scaled(1, 2)

    paired = Z in (3, 4)
    helper = jnp.logical_and(z <= Z - 3, paired)
    helped = jnp.logical_and(z >= 2, paired)

    def block_copies(j, a, send_sem, device):
        return (
            remote(kv_buf.at[j], kv_buf.at[j], send_sem.at[a, 0], kvrecv.at[j, 0], device),
            remote(cum_buf.at[j], cum_buf.at[j], send_sem.at[a, 1], kvrecv.at[j, 1], device),
        )

    def z_copies(dz):
        j = (z - dz) * X + x
        return block_copies(j, dz, zsend, {"sp": lax.rem(sp + X, SP)})

    def x_copies(dz, dx):
        j = (z - dz) * X + x
        xo = lax.rem(x + dx, X)
        return block_copies(j, dz, xsend.at[dx - 1], {"sp": z * X + xo})

    def for_sends(dz, own, act):
        if own or not paired:

            @pl.when(z < Z - 1)
            def _():
                for c in z_copies(dz):
                    act(c)

        for dx in range(1, X):
            if own:

                @pl.when(jnp.logical_or(lax.rem(x + dx, X) > x, helper))
                def _():
                    for c in x_copies(dz, dx):
                        act(c)
            else:
                for c in x_copies(dz, dx):
                    act(c)

    def kv_wait(j):
        for c in block_copies(j, 0, zsend, {"sp": lax.rem(sp + X, SP)}):
            c.wait_recv()

    for_sends(0, True, lambda c: c.start())

    q_ref[...] = scaled(4)
    q_copy = remote(
        q_ref, q_far, qsend.at[0], qrecv.at[0], {"sp": lax.rem(sp + SP - 2 * X, SP)}
    )

    @pl.when(helped)
    def _():
        q_copy.start()

    for i, (w, buf) in enumerate(((out_lru, wl_buf), (out_fox, wf_buf))):
        for k in range(1, TP):
            t = lax.rem(tp + k, TP)
            cols = pl.ds(pl.multiple_of(t * oc, 128), oc)
            s = remote(w.at[:, cols], buf.at[tp], wsend.at[i, k], wrecv.at[i, tp], {"tp": t})
            s.start()
            pending.append(s)

    gate_ref[...] = scaled(3)

    @pl.when(sp == 0)
    def _():
        pad[0:8, :] = jnp.zeros((8, lw), F32)

    @pl.when(sp > 0)
    def _():
        halo_copy.wait_recv()
        pad[0:8, :] = halo[...].astype(F32)[hb - 8 : hb, :]

    pad[8 : 8 + rows, :] = lru_ref[...].astype(F32)
    chans = pl.ds(pl.multiple_of(tp * lw, 128), lw)
    taps = conv_w.shape[0]
    taps_f32 = conv_w[:, chans].astype(F32)
    conv = jnp.zeros((rows, lw), F32)
    for j in range(taps):
        conv = conv + taps_f32[j : j + 1, :] * pad[8 - (taps - 1) + j : 8 - (taps - 1) + j + rows, :]
    conv_b = conv.astype(BF16)

    def sigmoid(v):
        return 1.0 / (1.0 + jnp.exp(-v))

    recur_gate = sigmoid(jnp.dot(conv_b, bd_r[...], preferred_element_type=F32))
    input_gate = sigmoid(jnp.dot(conv_b, bd_i[...], preferred_element_type=F32))
    own_rate = rate[:, chans]
    softplus = jnp.maximum(-own_rate, 0.0) + jnp.log1p(jnp.exp(-jnp.abs(own_rate)))
    for c in own_loads:
        c.wait()
    log_decay = -decay_sharpness * softplus * recur_gate + decay_buf[...]
    prefix_ref[...] = jnp.exp(log_decay)
    local_ref[...] = jnp.sqrt(one_minus_exp(2.0 * log_decay)) * input_gate * conv_b.astype(F32)
    row_id = lax.broadcasted_iota(jnp.int32, (rows, lw), 0)
    step = 1
    while step < rows:
        a = prefix_ref[...]
        b = local_ref[...]
        keep = row_id >= step
        a_prev = jnp.where(keep, pltpu.roll(a, step, 0), 1.0)
        b_prev = jnp.where(keep, pltpu.roll(b, step, 0), 0.0)
        local_ref[...] = b + a * b_prev
        prefix_ref[...] = a * a_prev
        step *= 2
    ends[sp, 0:1, :] = prefix_ref[rows - 1 : rows, :]
    ends[sp, 1:2, :] = local_ref[rows - 1 : rows, :]

    def end_copy(k):
        return remote(
            ends.at[sp], ends.at[sp], esend.at[k], erecv.at[sp], {"sp": lax.rem(sp + k, SP)}
        )

    for k in range(1, SP):

        @pl.when(sp + k < SP)
        def _():
            end_copy(k).start()

    score_scale = HEAD_DIM ** (-0.5)
    qc = rows // 2

    def attend(j, diagonal, far_first=None):
        other = far_first is not None
        first = diagonal or far_first
        qs, ms, ls, os = (q_far, m_far, l_far, o_far) if other else (q_ref, m_ref, l_ref, o_ref)

        def some(i, carry):
            r = pl.ds(pl.multiple_of(i * qc, qc), qc)
            for h in range(H):
                hs = slice(h * HEAD_DIM, (h + 1) * HEAD_DIM)
                vs = slice(fw + h * HEAD_DIM, fw + (h + 1) * HEAD_DIM)
                s = lax.dot_general(
                    qs[r, hs],
                    kv_buf[j, :, hs],
                    (((1,), (1,)), ((), ())),
                    preferred_element_type=F32,
                )
                s = s * score_scale
                if not other:
                    s = s + fcol[r, h : h + 1]
                s = s - cum_buf[j, h : h + 1, :]
                if diagonal:
                    causal = (
                        lax.broadcasted_iota(jnp.int32, (qc, rows), 0) + i * qc
                        >= lax.broadcasted_iota(jnp.int32, (qc, rows), 1)
                    )
                    s = jnp.where(causal, s, -1e30)
                top = jnp.max(s, axis=1, keepdims=True)
                if first:
                    p = jnp.exp(s - top)
                    ms[h, r, :] = top
                    ls[h, r, :] = jnp.sum(p, axis=1, keepdims=True)
                    os[h, r, :] = jnp.dot(
                        p.astype(BF16), kv_buf[j, :, vs], preferred_element_type=F32
                    )
                else:
                    old = ms[h, r, :]
                    new = jnp.maximum(old, top)
                    p = jnp.exp(s - new)
                    fade = jnp.exp(old - new)
                    ms[h, r, :] = new
                    ls[h, r, :] = ls[h, r, :] * fade + jnp.sum(p, axis=1, keepdims=True)
                    os[h, r, :] = os[h, r, :] * fade + jnp.dot(
                        p.astype(BF16), kv_buf[j, :, vs], preferred_element_type=F32
                    )
            return carry

        lax.fori_loop(0, rows // qc, some, 0)

    attend(sp, True)

    def row_blocks(dz):
        for dx in range(1, X):
            xo = lax.rem(x + dx, X)

            @pl.when(jnp.logical_or(dz > 0, xo < x))
            def _():
                j = (z - dz) * X + xo
                kv_wait(j)
                attend(j, False)

    def finish_lru():
        incoming[...] = jnp.zeros_like(incoming)
        for j in range(SP - 1):

            @pl.when(j < sp)
            def _():
                remote(
                    ends.at[j], ends.at[j], esend.at[0], erecv.at[j], {"sp": lax.rem(sp + 1, SP)}
                ).wait_recv()
                incoming[...] = ends[j, 0:1, :] * incoming[...] + ends[j, 1:2, :]

        states = local_ref[...] + prefix_ref[...] * incoming[...]
        g = gate_ref[...].astype(F32)
        gelu = 0.5 * g * (1.0 + jnp.tanh(0.7978845608028654 * (g + 0.044715 * (g * g * g))))
        br_lru[tp] = (states * gelu).astype(BF16)
        for k in range(Y - 1, -1, -1):
            lru_copy(k).start()

    def lru_copy(k):
        to = far[k] if k else partner
        return remote(br_lru.at[tp], br_lru.at[tp], lsend.at[k], lrecv.at[tp], {"tp": to})

    lru_step = min(2, Z - 1)
    if Z == 1:
        finish_lru()

    def hop(dz, carry):
        @pl.when(dz <= z)
        def _():
            j = (z - dz) * X + x
            kv_wait(j)
            for_sends(dz, False, lambda c: c.start())
            row_blocks(dz - 1)
            attend(j, False)

        @pl.when(dz == lru_step)
        def _():
            finish_lru()

        return carry

    up = {"sp": lax.rem(sp + 2 * X, SP)}
    part_copies = (
        remote(part_out, part_in, osend.at[0], orecv.at[0], up),
        remote(stat_out, stat_in, osend.at[1], orecv.at[1], up),
    )

    def send_partial():
        for h in range(H):
            part_out[:, h * HEAD_DIM : (h + 1) * HEAD_DIM] = o_far[h].astype(BF16)
            cum_pad[:, h : h + 1] = m_far[h]
            cum_pad[:, H + h : H + h + 1] = l_far[h]
        stat_out[...] = cum_pad[...].T[0:8, :]
        for c in part_copies:
            c.start()

    if paired:
        below = (z - 1) * X

        @pl.when(helper)
        def _():
            q_copy.wait_recv()
            attend(sp, False, True)

        @pl.when(z >= 1)
        def _():
            kv_wait(below + x)
            for_sends(1, False, lambda c: c.start())

        for dx in range(1, X):
            xo = lax.rem(x + dx, X)

            @pl.when(jnp.logical_or(xo < x, helper))
            def _():
                kv_wait(z * X + xo)

            @pl.when(helper)
            def _():
                attend(z * X + xo, False, False)

        @pl.when(jnp.logical_and(helper, z == 0))
        def _():
            send_partial()

        for dx in range(1, X):
            xo = lax.rem(x + dx, X)

            @pl.when(xo < x)
            def _():
                attend(z * X + xo, False)

        finish_lru()

        @pl.when(jnp.logical_and(helper, z >= 1))
        def _():
            attend(below + x, False, False)

        @pl.when(z >= 1)
        def _():
            attend(below + x, False)
            for dx in range(1, X):
                j = below + lax.rem(x + dx, X)
                kv_wait(j)

                @pl.when(helper)
                def _():
                    attend(j, False, False)

            @pl.when(helper)
            def _():
                send_partial()

            for dx in range(1, X):
                attend(below + lax.rem(x + dx, X), False)

    else:
        lax.fori_loop(1, Z, hop, 0)

    def lru_wait(t):
        remote(br_lru.at[t], br_lru.at[t], lsend.at[0], lrecv.at[t], {"tp": partner}).wait_recv()

    def lru_dot(t):
        return jnp.dot(br_lru[t], wl_buf[t], preferred_element_type=F32)

    oacc[...] = lru_dot(tp)
    for k in range(1, TP):
        t = lax.rem(tp + k, TP)
        for i, buf in enumerate((wl_buf, wf_buf)):
            remote(buf.at[t], buf.at[t], wsend.at[i, k], wrecv.at[i, t], {"tp": t}).wait_recv()
    for k in range(1, Y):
        lru_wait(far[k])
        ref = br_lru.at[far[k]]
        s = remote(ref, ref, lfwd.at[k], lrecv.at[far[k]], {"tp": partner})
        s.start()
        pending.append(s)
    lru_wait(partner)
    oacc[...] += lru_dot(partner)
    for k in range(1, Y):
        oacc[...] += lru_dot(far[k])
        lru_wait(pfar[k])
        oacc[...] += lru_dot(pfar[k])

    if paired:

        @pl.when(helped)
        def _():
            for c in part_copies:
                c.wait_recv()
            wide[0:8, :] = stat_in[...]
            stats = wide[...].T
            for h in range(H):
                m_in = stats[:, h : h + 1] + fcol[:, h : h + 1]
                l_in = stats[:, H + h : H + h + 1]
                part = part_in[:, h * HEAD_DIM : (h + 1) * HEAD_DIM].astype(F32)
                new = jnp.maximum(m_ref[h], m_in)
                fade = jnp.exp(m_ref[h] - new)
                grow = jnp.exp(m_in - new)
                l_ref[h] = l_ref[h] * fade + l_in * grow
                o_ref[h] = o_ref[h] * fade + part * grow

    else:
        row_blocks(z)

    for c in range(CH):
        r = chunk(c)
        for h in range(H):
            br_fox[tp, r, h * HEAD_DIM : (h + 1) * HEAD_DIM] = (
                o_ref[h, r, :] / l_ref[h, r, :]
            ).astype(BF16)
        ref = br_fox.at[tp, r]
        for k in list(range(1, Y)) + [0]:
            to = far[k] if k else partner
            s = remote(ref, ref, fsend.at[k, c], frecv.at[tp, c], {"tp": to})
            s.start()
            pending.append(s)

    def fox_wait(src, c):
        ref = br_fox.at[src, chunk(c)]
        remote(ref, ref, fsend.at[0, c], frecv.at[src, c], {"tp": partner}).wait_recv()

    def fox_dot(src, r):
        return jnp.dot(br_fox[src, r, :], wf_buf[src], preferred_element_type=F32)

    for c in range(CH):
        fox_wait(partner, c)
        oacc[chunk(c), :] += fox_dot(tp, chunk(c)) + fox_dot(partner, chunk(c))
    for c in range(CH):
        r = chunk(c)
        for k in range(1, Y):
            fox_wait(far[k], c)
            ref = br_fox.at[far[k], r]
            s = remote(ref, ref, ffwd.at[k, c], frecv.at[far[k], c], {"tp": partner})
            s.start()
            pending.append(s)
            oacc[r, :] += fox_dot(far[k], r)
        for k in range(1, Y):
            fox_wait(pfar[k], c)
            oacc[r, :] += fox_dot(pfar[k], r)
        out[r, :] = oacc[r, :].astype(out.dtype)

    for s in pending:
        s.wait_send()
    for k in range(Y):
        lru_copy(k).wait_send()

    @pl.when(helped)
    def _():
        q_copy.wait_send()

    @pl.when(helper)
    def _():
        for c in part_copies:
            c.wait_send()

    @pl.when(sp < SP - 1)
    def _():
        halo_copy.wait_send()

    for k in range(1, SP):

        @pl.when(sp + k < SP)
        def _():
            end_copy(k).wait_send()

    for_sends(0, True, lambda c: c.wait_send())

    def drain(dz, carry):
        @pl.when(dz <= z)
        def _():
            for_sends(dz, False, lambda c: c.wait_send())

        return carry

    if paired:

        @pl.when(z >= 1)
        def _():
            for_sends(1, False, lambda c: c.wait_send())

    else:
        lax.fori_loop(1, Z, drain, 0)


def shards(SP, TP, X, *args):
    tokens, lru_in, gate_in, query_w = args[:4]
    (conv_weight, rg_w, ig_w, rate, decay_extra, forget, out_lru, out_fox) = args[6:]
    rows, dcols = tokens.shape
    D, lw = lru_in.shape
    fw = query_w.shape[1]
    oc = out_lru.shape[1] // TP
    tot = 2 * lw + 3 * fw
    H = fw // HEAD_DIM
    Y = TP // 2
    Z = SP // X
    CH = 4
    vm = pl.BlockSpec(memory_space=pltpu.VMEM)
    hbm = pl.BlockSpec(memory_space=pl.ANY)
    dma = pltpu.SemaphoreType.DMA
    V = pltpu.VMEM
    scratch = [
        V((TP, rows, dcols), BF16),
        V((D, tot), BF16),
        V((rows, tot), F32),
        V((rows, 1), F32),
        V((rows, lw), BF16),
        V((16, lw), BF16),
        V((rows + 8, lw), F32),
        V((lw, lw), BF16),
        V((lw, lw), BF16),
        V((rows, lw), BF16),
        V((rows, fw), BF16),
        V((rows, lw), F32),
        V((rows, lw), F32),
        V((rows, lw), F32),
        V((SP, 8, lw), F32),
        V((1, lw), F32),
        V((SP, rows, 2 * fw), BF16),
        V((SP, 8, rows), F32),
        V((rows, 128), F32),
        V((128, rows), F32),
        V((rows, 128), F32),
        V((H, rows, 1), F32),
        V((H, rows, 1), F32),
        V((H, rows, HEAD_DIM), F32),
        V((rows, fw), BF16),
        V((H, rows, 1), F32),
        V((H, rows, 1), F32),
        V((H, rows, HEAD_DIM), F32),
        V((rows, fw), BF16),
        V((8, rows), F32),
        V((rows, fw), BF16),
        V((8, rows), F32),
        V((TP, lw, oc), BF16),
        V((TP, fw, oc), BF16),
        V((TP, rows, lw), BF16),
        V((TP, rows, fw), BF16),
        V((rows, oc), F32),
        dma((8,)),
        dma((Y, CH)),
        dma((Y, CH)),
        dma((TP, CH)),
        dma((1,)),
        dma((1,)),
        dma((SP,)),
        dma((SP,)),
        dma((Z, 2)),
        dma((max(X - 1, 1), Z, 2)),
        dma((SP, 2)),
        dma((2, TP)),
        dma((2, TP)),
        dma((TP,)),
        dma((TP,)),
        dma((Y, CH)),
        dma((Y, CH)),
        dma((TP, CH)),
        dma((Y,)),
        dma((1,)),
        dma((1,)),
        dma((2,)),
        dma((2,)),
    ]
    return pl.pallas_call(
        functools.partial(kernel, SP, TP, X),
        out_shape=jax.ShapeDtypeStruct((rows, oc), BF16),
        in_specs=[vm] + [hbm] * 5 + [vm] * 4 + [hbm, vm, hbm, hbm],
        out_specs=vm,
        scratch_shapes=scratch,
        compiler_params=pltpu.CompilerParams(
            collective_id=0, has_side_effects=True, vmem_limit_bytes=60 * 1024 * 1024
        ),
    )(*args[:9], rate.reshape(1, -1), decay_extra, forget.T, out_lru, out_fox)


def columns_of(mesh):
    SP = mesh.shape["sp"]
    try:
        X = len({d.coords[0] for d in mesh.devices.flat})
    except AttributeError:
        X = 2
    return X if SP % X == 0 else 1


def solution(mesh):
    placed = (
        P("sp", "tp"),
        P(None, "tp"),
        P(None, "tp"),
        P(None, "tp"),
        P(None, "tp"),
        P(None, "tp"),
        P(),
        P(),
        P(),
        P(),
        P("sp", "tp"),
        P("sp", "tp"),
        P("tp", None),
        P("tp", None),
    )
    body = functools.partial(shards, mesh.shape["sp"], mesh.shape["tp"], columns_of(mesh))
    return jax.shard_map(
        body, mesh=mesh, in_specs=placed, out_specs=P("sp", "tp"), check_vma=False
    )
```
